32 devices in a mesh: ep: 8 (over z, x), tp: 4 (over y, core).
Axes of the slice: x: 2, y: 2, z: 4, core: 2. Of those that a mesh axis runs over, the one named last changes fastest.
Arguments:
- mixer_input: bfloat16 [2048, 2048], P('ep'), may hold values from -6 to 6
- mixer_gain: float32 [2048], replicated, may hold values from 0.1 to 8
- query_one: bfloat16 [2048, 512], P(None, 'tp'), may hold values from -0.1875 to 0.1875
- query_two: bfloat16 [2048, 512], P(None, 'tp'), may hold values from -0.1875 to 0.1875
- key_one: bfloat16 [2048, 256], P(None, 'tp'), may hold values from -0.1875 to 0.1875
- key_two: bfloat16 [2048, 256], P(None, 'tp'), may hold values from -0.1875 to 0.1875
- value_weight: bfloat16 [2048, 512], P(None, 'tp'), may hold values from -0.125 to 0.125
- lambdas: float32 [8], P('tp'), may hold values from 0.3 to 0.8
- head_gain: float32 [128], replicated, may hold values from 0.1 to 1.9
- output_weight: bfloat16 [1024, 2048], P('tp'), may hold values from -0.1875 to 0.1875
- expert_input: bfloat16 [4096, 2048], P(('ep', 'tp')), may hold values from -6 to 6
- expert_gain: float32 [2048], replicated, may hold values from 0.1 to 1.9
- routes: int32 [4096, 2], P(('ep', 'tp')), may hold values from 0 to 7, all different within a row; in each aligned block of 128 rows (0 to 127, 128 to 255, ...) at most 40 rows name the same one
- route_weight: float32 [4096, 2], P(('ep', 'tp')), may hold values from 0.2 to 1
- expert_gate: bfloat16 [8, 2048, 1024], P('ep', None, 'tp'), may hold values from -0.125 to 0.125
- expert_up: bfloat16 [8, 2048, 1024], P('ep', None, 'tp'), may hold values from -0.125 to 0.125
- expert_down: bfloat16 [8, 1024, 2048], P('ep', 'tp'), may hold values from -0.1875 to 0.1875
- shared_gate: bfloat16 [2048, 512], P(None, 'tp'), may hold values from -0.125 to 0.125
- shared_up: bfloat16 [2048, 512], P(None, 'tp'), may hold values from -0.125 to 0.125
- shared_down: bfloat16 [512, 2048], P('tp'), may hold values from -0.25 to 0.25
Outputs:
- mixer_output: bfloat16 [2048, 2048], P(('ep', 'tp'))
- expert_output: bfloat16 [4096, 2048], P(('ep', 'tp'))
The draws below stay inside these ranges and needn't reach their ends.
Inputs may be any that keep to these rules, and one draw needn't show every extreme that they name: `routes`: each row names 2 different experts; in the rows of one device no expert is named by more than 40 rows, and some device names some expert exactly 40 times.
All inputs are finite; a program needn't handle non-finite values.
Results may differ from the reference program's by a relative error of at most 0.014.
The reference program's roundings to bfloat16 on the way count: a program that leaves them out, or rounds other values in their place, can miss the bound.
Values may be sent and summed in bfloat16 or wider, within the bound.
No kernel may reach another device: no remote copies, remote signals or barrier semaphores. Data moves between devices by JAX's collectives and lax.ppermute only.
A program may use at most 128 MiB of HBM per device.

```python
import math
import jax
import jax.numpy as jnp
import numpy as np
from jax import lax

D = 2048
HEADS = 8
KV_HEADS = 4
HEAD = 64
VDIM = 128
EFF = 1024
SFF = 512
TOP = 2
EXPERTS = 8
ROWS = 128
CAP = 40
SEQ_LEN = 2048
TOKENS = 4096
N_EP = 8
N_TP = 4


def draw_mixer_gain(key, part):
    return jnp.clip(1.0 + 0.18 * jax.random.normal(key, (D,), jnp.float32), 0.1, 1.9)


def shard_levels(stream_key, shape, cuts, least, largest):
    def one(position, blocks):
        draws = jax.random.uniform(jax.random.fold_in(jax.random.fold_in(stream_key, 6), position), (blocks,), jnp.float32, least / len(cuts), largest / len(cuts))
        return jnp.repeat(jnp.exp(draws), shape[position] // blocks).reshape((-1,) + (1,) * (len(shape) - position - 1))

    level = one(*cuts[0])
    for cut in cuts[1:]:
        level = level * one(*cut)
    return level


def deal_out(own_key, own, number, rows, number_of, top, most, slope):
    sequence = jax.random.permutation(own_key, number_of)
    crowded, common = shares(number_of, rows * top, most, slope, True), shares(number_of, rows * top, most, slope, False)
    places = jnp.arange(number_of)

    def named(tallies, offset_by):
        used = int((tallies > 0).sum())
        fixed = max(1, used // 4)
        moved = fixed + (places - fixed + offset_by * (used - fixed)) % max(1, number_of - fixed)
        return jnp.zeros((number_of,), jnp.int32).at[sequence[jnp.where(places < fixed, places, moved)]].set(jnp.asarray(tallies, jnp.int32))

    tallies = jnp.where(number % 4 == 0, named(crowded, number // 4), named(common, number - number // 4 - 1))
    mixed = jax.random.permutation(jax.random.fold_in(own, 3), number_of)
    giver, sink = mixed[0:number_of // 2 * 2:2], mixed[1:number_of // 2 * 2:2]
    slack = jnp.minimum(tallies[giver] - 1, most - tallies[sink]) // 2
    slack = jnp.where((giver == sequence[0]) | (sink == sequence[0]) | (tallies[sink] == 0), 0, jnp.maximum(slack, 0))
    moved = jax.random.randint(jax.random.fold_in(own, 4), (number_of // 2,), 0, 1 << 20) % (slack + 1)
    tallies = tallies.at[giver].add(-moved).at[sink].add(moved)
    items = jnp.searchsorted(jnp.cumsum(tallies), jnp.arange(rows * top), side="right").astype(jnp.int32)
    listing = items.reshape(top, rows).T
    listing = listing[jax.random.permutation(jax.random.fold_in(own, 1), rows)]
    offset_by = jax.random.randint(jax.random.fold_in(own, 2), (rows, 1), 0, top)
    return jnp.take_along_axis(listing, (jnp.arange(top)[None, :] + offset_by) % top, axis=1)


def shares(count, total, reach, slope, full):
    loads = [(1 << 20) // math.isqrt(standing ** slope) + 1 for standing in range(1, count + 1)]
    largest = reach if full else min(reach, max(-(-total // count), total * loads[0] // sum(loads)))
    least = 1 if total - largest >= count - 1 else 0
    given, surplus = [largest] + [least] * (count - 1), total - largest - least * (count - 1)
    while surplus > 0:
        free = [i for i in range(1, count) if given[i] < largest] or [i for i in range(1, count) if given[i] < reach]
        whole, budget = sum([loads[i] for i in free]), surplus
        for i in free:
            extra = min(reach - given[i], max(1, budget * loads[i] // whole), surplus)
            given[i] = given[i] + extra
            surplus = surplus - extra
    return np.array(given)


def centred(rng, dims, width, most, shards=(), kind=jnp.bfloat16):
    drawn = width * jax.random.normal(rng, dims, jnp.float32)
    if shards:
        drawn = drawn * shard_levels(rng, dims, shards, -0.22, 0.18)
    return jnp.clip(drawn, -most, most).astype(kind)


def setup_inputs(seed: int = 0) -> dict:
    arg_keys = jax.random.split(jax.random.key(seed), 21)
    mixer_input = centred(arg_keys[0], (SEQ_LEN, D), 1.0, 6.0, ((0, 8),))
    mixer_gain = draw_mixer_gain(jax.random.fold_in(arg_keys[20], 71), 0)
    query_one = centred(arg_keys[2], (D, HEADS * HEAD), (D // 2) ** -0.5, 0.1875, ((1, 4),))
    query_two = centred(arg_keys[3], (D, HEADS * HEAD), (D // 2) ** -0.5, 0.1875, ((1, 4),))
    key_one = centred(arg_keys[4], (D, KV_HEADS * HEAD), (D // 2) ** -0.5, 0.1875, ((1, 4),))
    key_two = centred(arg_keys[5], (D, KV_HEADS * HEAD), (D // 2) ** -0.5, 0.1875, ((1, 4),))
    value_weight = centred(arg_keys[6], (D, KV_HEADS * VDIM), D ** -0.5, 0.125, ((1, 4),))
    lambdas = jnp.clip(0.3 + 0.5 * jax.random.uniform(arg_keys[7], (HEADS,), jnp.float32) ** shard_levels(arg_keys[7], (HEADS,), ((0, 4),), -0.2, 0.2), 0.3, 0.8)
    head_gain = jnp.clip(1.0 + 0.18 * jax.random.normal(arg_keys[8], (VDIM,), jnp.float32), 0.1, 1.9)
    output_weight = centred(arg_keys[9], (HEADS * VDIM, D), (HEADS * VDIM) ** -0.5, 0.1875, ((0, 4),))
    expert_input = centred(arg_keys[10], (TOKENS, D), 1.0, 6.0, ((0, 32),))
    expert_gain = jnp.clip(1.0 + 0.18 * jax.random.normal(arg_keys[11], (D,), jnp.float32), 0.1, 1.9)
    routes_keys = jax.random.split(jax.random.fold_in(arg_keys[12], 1), TOKENS // ROWS)
    routes_turns = jax.random.permutation(jax.random.fold_in(arg_keys[12], 3), TOKENS // ROWS)
    routes = jax.vmap(lambda own, number: deal_out(jax.random.fold_in(arg_keys[12], 2), own, number, ROWS, EXPERTS, TOP, CAP, 2))(routes_keys, routes_turns).reshape((TOKENS, TOP))
    route_weight = jnp.clip(jnp.exp(math.log(1.0) - 1.609438 * jax.random.uniform(arg_keys[13], (TOKENS, TOP), jnp.float32) ** shard_levels(arg_keys[13], (TOKENS, TOP), ((0, 32),), -0.2, 0.2)), 0.2, 1.0)
    expert_gate = centred(arg_keys[14], (EXPERTS, D, EFF), D ** -0.5, 0.125, ((0, 8), (2, 4)))
    expert_up = centred(arg_keys[15], (EXPERTS, D, EFF), D ** -0.5, 0.125, ((0, 8), (2, 4)))
    expert_down = centred(arg_keys[16], (EXPERTS, EFF, D), EFF ** -0.5, 0.1875, ((0, 8), (1, 4)))
    shared_gate = centred(arg_keys[17], (D, SFF), D ** -0.5, 0.125, ((1, 4),))
    shared_up = centred(arg_keys[18], (D, SFF), D ** -0.5, 0.125, ((1, 4),))
    shared_down = centred(arg_keys[19], (SFF, D), SFF ** -0.5, 0.25, ((0, 4),))
    return dict(mixer_input=mixer_input, mixer_gain=mixer_gain, query_one=query_one, query_two=query_two, key_one=key_one, key_two=key_two, value_weight=value_weight, lambdas=lambdas, head_gain=head_gain, output_weight=output_weight, expert_input=expert_input, expert_gain=expert_gain, routes=routes, route_weight=route_weight, expert_gate=expert_gate, expert_up=expert_up, expert_down=expert_down, shared_gate=shared_gate, shared_up=shared_up, shared_down=shared_down)


EPS = 1e-06
NEG = -1e+30

def normalize(activations, scaling):
    values = activations.astype(jnp.float32)
    factor = lax.rsqrt(lax.optimization_barrier(jnp.mean(values * values, axis=-1, keepdims=True)) + EPS)
    return (values * factor * scaling).astype(jnp.bfloat16)

def swiglu(inputs, gate_weight, up_weight):
    gated = jnp.dot(inputs, gate_weight, preferred_element_type=jnp.float32)
    lifted = jnp.dot(inputs, up_weight, preferred_element_type=jnp.float32)
    return (jax.nn.silu(gated) * lifted).astype(jnp.bfloat16)

def quarter_sum(hidden, down_weight):
    group_width = hidden.shape[1] // N_TP
    running_sum = jnp.zeros((hidden.shape[0], down_weight.shape[1]), jnp.float32)
    for group_index in range(N_TP):
        partial_product = jnp.dot(hidden[:, group_index * group_width:(group_index + 1) * group_width], down_weight[group_index * group_width:(group_index + 1) * group_width], preferred_element_type=jnp.float32)
        rounded = lax.optimization_barrier(partial_product.astype(jnp.bfloat16))
        running_sum = running_sum + rounded.astype(jnp.float32)
    return running_sum

def attention(mixer_input, mixer_gain, query_one, query_two, key_one, key_two, value_weight, lambdas, head_gain, output_weight):
    normed = normalize(mixer_input, mixer_gain)
    tokens = normed.shape[0]
    group_size = HEADS // KV_HEADS

    def project(weight):
        return jnp.dot(normed, weight, preferred_element_type=jnp.float32).astype(jnp.bfloat16)
    query_first = project(query_one).reshape(tokens, KV_HEADS, group_size, HEAD)
    query_second = project(query_two).reshape(tokens, KV_HEADS, group_size, HEAD)
    key_first = project(key_one).reshape(tokens, KV_HEADS, HEAD).astype(jnp.float32)
    key_second = project(key_two).reshape(tokens, KV_HEADS, HEAD).astype(jnp.float32)
    value_rows = project(value_weight).reshape(tokens, KV_HEADS, VDIM).astype(jnp.float32)
    lambda_grid = lambdas.reshape(KV_HEADS, group_size)[:, :, None, None]
    key_pos = jnp.arange(tokens, dtype=jnp.int32)
    span_rows = min(128, tokens)

    def single_map(queries, key_rows, visible):
        scores = jnp.einsum('qkgd,jkd->kgqj', queries.astype(jnp.float32), key_rows) * HEAD ** (-0.5)
        scores = jnp.where(visible, scores, NEG)
        highest = lax.optimization_barrier(jnp.max(scores, axis=-1, keepdims=True))
        weights = jnp.where(visible, jnp.exp(scores - highest), 0.0)
        totals = lax.optimization_barrier(jnp.sum(weights, axis=-1))
        rounded = lax.optimization_barrier(weights.astype(jnp.bfloat16)).astype(jnp.float32)
        mixed = jnp.einsum('kgqj,jkd->kgqd', rounded, value_rows)
        return mixed / totals[..., None]

    def query_block(block_index):
        offset = (block_index * span_rows).astype(jnp.int32)
        query_pos = offset + jnp.arange(span_rows, dtype=jnp.int32)
        visible = key_pos[None, :] <= query_pos[:, None]
        first_part = single_map(lax.dynamic_slice_in_dim(query_first, offset, span_rows, 0), key_first, visible)
        second_part = single_map(lax.dynamic_slice_in_dim(query_second, offset, span_rows, 0), key_second, visible)
        combined = first_part - lambda_grid * second_part
        factor = lax.rsqrt(lax.optimization_barrier(jnp.mean(combined * combined, axis=-1, keepdims=True)) + EPS)
        normed_heads = (combined * factor * head_gain).astype(jnp.bfloat16)
        return normed_heads.transpose(2, 0, 1, 3).reshape(span_rows, HEADS * VDIM)
    head_rows = lax.map(query_block, jnp.arange(tokens // span_rows, dtype=jnp.int32))
    head_rows = head_rows.reshape(tokens, HEADS * VDIM)
    return quarter_sum(head_rows, output_weight).astype(jnp.bfloat16)

def experts_part(expert_input, expert_gain, routes, route_weight, expert_gate, expert_up, expert_down, shared_gate, shared_up, shared_down):
    normed = normalize(expert_input, expert_gain)
    tokens = normed.shape[0]
    shared_result = quarter_sum(swiglu(normed, shared_gate, shared_up), shared_down)
    flat_routes = routes.reshape(-1).astype(jnp.int32)
    copies = flat_routes.shape[0]
    onehot = (flat_routes[:, None] == jnp.arange(EXPERTS, dtype=jnp.int32)[None, :]).astype(jnp.int32)
    slot_place = lax.optimization_barrier(jnp.sum((jnp.cumsum(onehot, axis=0) - onehot) * onehot, axis=1)).astype(jnp.int32)
    owners = (jnp.arange(copies, dtype=jnp.int32) // TOP).astype(jnp.int32)
    table = jnp.zeros((EXPERTS, N_EP * N_TP * CAP), jnp.int32).at[flat_routes, slot_place].set(owners)

    def one_expert(expert_index):
        chosen = normed[table[expert_index]]
        hidden = swiglu(chosen, expert_gate[expert_index], expert_up[expert_index])
        return quarter_sum(hidden, expert_down[expert_index]).astype(jnp.bfloat16)
    results = lax.map(one_expert, jnp.arange(EXPERTS, dtype=jnp.int32))
    picked = results[flat_routes, slot_place].astype(jnp.float32).reshape(tokens, TOP, -1)
    routed = lax.optimization_barrier(jnp.sum(picked * route_weight[:, :, None], axis=1))
    return (routed + shared_result).astype(jnp.bfloat16)

def reference(mixer_input, mixer_gain, query_one, query_two, key_one, key_two, value_weight, lambdas, head_gain, output_weight, expert_input, expert_gain, routes, route_weight, expert_gate, expert_up, expert_down, shared_gate, shared_up, shared_down):
    mixer_output = attention(mixer_input, mixer_gain, query_one, query_two, key_one, key_two, value_weight, lambdas, head_gain, output_weight)
    expert_output = experts_part(expert_input, expert_gain, routes, route_weight, expert_gate, expert_up, expert_down, shared_gate, shared_up, shared_down)
    return (mixer_output, expert_output)
```

```python
import jax
import jax.numpy as jnp
from jax import lax
from jax.experimental import pallas as pl
from jax.experimental.pallas import tpu as pltpu
from jax.sharding import PartitionSpec as P

HEAD = 64
EPS = 1e-06
NEG = -1e30
MOST_PERMUTES = 8


def normalize(activations, scaling):
    values = activations.astype(jnp.float32)
    factor = lax.rsqrt(jnp.mean(values * values, axis=-1, keepdims=True) + EPS)
    return (values * factor * scaling).astype(jnp.bfloat16)


def rotate(chunk, axis, size, shift):
    return lax.ppermute(chunk, axis, [(i, (i + shift) % size) for i in range(size)])


def exchange(chunks, rank, size, sign):
    if size <= MOST_PERMUTES:
        return [chunks[0]] + [
            rotate(chunk, "ep", size, sign * k) for k, chunk in enumerate(chunks) if k
        ]
    order = (sign * (jnp.arange(size, dtype=jnp.int32) - rank)) % size
    arrived = lax.all_to_all(
        jnp.stack(chunks)[order], "ep", split_axis=0, concat_axis=0, tiled=True
    )
    back = (rank - sign * jnp.arange(size, dtype=jnp.int32)) % size
    arrived = arrived[back]
    return [arrived[k] for k in range(size)]


def tp_blocks(shard, size):
    blocks = [shard]
    bit = size // 2
    while bit:
        pairs = [(i, i ^ bit) for i in range(size)]
        blocks = blocks + [lax.ppermute(block, "tp", pairs) for block in blocks]
        bit //= 2
    return blocks


def attention_kernel(
    rank_ref,
    lambda_ref,
    query_ref,
    own_ref,
    others_ref,
    gain_ref,
    weight_ref,
    out_ref,
    maxima,
    totals,
    weighted,
    *,
    local_kv,
    group,
    value_dim,
):
    rows = query_ref.shape[0]
    key_cols = local_kv * HEAD
    query_cols = key_cols * group

    def stacked(head, which):
        first = which * query_cols + head * group * HEAD
        return jnp.concatenate(
            [query_ref[:, first + g * HEAD : first + (g + 1) * HEAD] for g in range(group)], axis=0
        ) * jnp.bfloat16(HEAD ** (-0.5))

    queries = [[stacked(head, which) for which in range(2)] for head in range(local_kv)]

    def block(keys, head, which):
        key_part = keys[:, which * key_cols + head * HEAD : which * key_cols + (head + 1) * HEAD]
        value_part = keys[
            :, 2 * key_cols + head * value_dim : 2 * key_cols + (head + 1) * value_dim
        ]
        scores = lax.dot_general(
            queries[head][which],
            key_part,
            (((1,), (1,)), ((), ())),
            preferred_element_type=jnp.float32,
        )
        return scores, value_part

    own = own_ref[...]
    position = lax.broadcasted_iota(jnp.int32, (group * rows, rows), 0) % rows
    visible = lax.broadcasted_iota(jnp.int32, (group * rows, rows), 1) <= position
    for head in range(local_kv):
        for which in range(2):
            slot = head * 2 + which
            scores, value_part = block(own, head, which)
            scores = jnp.where(visible, scores, NEG)
            highest = jnp.max(scores, axis=-1, keepdims=True)
            weights = jnp.exp(scores - highest)
            maxima[slot] = highest
            totals[slot] = jnp.sum(weights, axis=-1, keepdims=True)
            weighted[slot] = jnp.dot(
                weights.astype(jnp.bfloat16), value_part, preferred_element_type=jnp.float32
            )

    def earlier_block(step, carry):
        keys = others_ref[step]
        for head in range(local_kv):
            for which in range(2):
                slot = head * 2 + which
                scores, value_part = block(keys, head, which)
                before = maxima[slot]
                highest = jnp.maximum(before, jnp.max(scores, axis=-1, keepdims=True))
                shrink = jnp.exp(before - highest)
                weights = jnp.exp(scores - highest)
                maxima[slot] = highest
                totals[slot] = totals[slot] * shrink + jnp.sum(weights, axis=-1, keepdims=True)
                weighted[slot] = weighted[slot] * shrink + jnp.dot(
                    weights.astype(jnp.bfloat16), value_part, preferred_element_type=jnp.float32
                )
        return carry

    lax.fori_loop(0, rank_ref[0], earlier_block, 0)
    parts = []
    for head in range(local_kv):
        first = weighted[head * 2] / totals[head * 2]
        second = weighted[head * 2 + 1] / totals[head * 2 + 1]
        for g in range(group):
            span = slice(g * rows, (g + 1) * rows)
            combined = first[span] - lambda_ref[head * group + g] * second[span]
            factor = lax.rsqrt(jnp.mean(combined * combined, axis=-1, keepdims=True) + EPS)
            parts.append((combined * factor * gain_ref[...]).astype(jnp.bfloat16))
    head_rows = jnp.concatenate(parts, axis=1)
    out_ref[...] = jnp.dot(
        head_rows, weight_ref[...], preferred_element_type=jnp.float32
    ).astype(jnp.bfloat16)


def attention(rank, lambdas, queries, own, others, head_gain, output_weight, local_kv, group):
    rows = queries.shape[0]
    value_dim = head_gain.shape[0]
    kernel = lambda *refs: attention_kernel(
        *refs, local_kv=local_kv, group=group, value_dim=value_dim
    )
    smem = pl.BlockSpec(memory_space=pltpu.SMEM)
    vmem = pl.BlockSpec(memory_space=pltpu.VMEM)
    stats = (2 * local_kv, group * rows, 1)
    return pl.pallas_call(
        kernel,
        out_shape=jax.ShapeDtypeStruct((rows, output_weight.shape[1]), jnp.bfloat16),
        in_specs=[smem, smem] + [vmem] * 5,
        out_specs=vmem,
        scratch_shapes=[
            pltpu.VMEM(stats, jnp.float32),
            pltpu.VMEM(stats, jnp.float32),
            pltpu.VMEM((2 * local_kv, group * rows, value_dim), jnp.float32),
        ],
        cost_estimate=pl.CostEstimate(
            flops=6_000_000_000, transcendentals=4_000_000, bytes_accessed=4_000_000
        ),
        name="attention",
    )(rank.reshape(1), lambdas, queries, own, others, head_gain.reshape(1, -1), output_weight)


def combine_kernel(slot_ref, weight_ref, returned_ref, shared_ref, out_ref):
    slot_count = returned_ref.shape[0]
    tokens, top = slot_ref.shape
    places = lax.broadcasted_iota(jnp.int32, (tokens, slot_count), 1)
    total = shared_ref[...].astype(jnp.float32)
    for k in range(top):
        chosen = (places == slot_ref[:, k : k + 1]).astype(jnp.float32).astype(jnp.bfloat16)
        picked = jnp.dot(chosen, returned_ref[...], preferred_element_type=jnp.float32)
        total = total + picked * weight_ref[:, k : k + 1]
    out_ref[...] = total.astype(jnp.bfloat16)


def combine(slot_ids, route_weight, returned, shared):
    tokens, width = shared.shape
    slot_count = returned.shape[0]
    top = slot_ids.shape[1]
    cols = width // 4
    return pl.pallas_call(
        combine_kernel,
        grid=(width // cols,),
        out_shape=jax.ShapeDtypeStruct((tokens, width), jnp.bfloat16),
        in_specs=[
            pl.BlockSpec((tokens, top), lambda i: (0, 0)),
            pl.BlockSpec((tokens, top), lambda i: (0, 0)),
            pl.BlockSpec((slot_count, cols), lambda i: (0, i)),
            pl.BlockSpec((tokens, cols), lambda i: (0, i)),
        ],
        out_specs=pl.BlockSpec((tokens, cols), lambda i: (0, i)),
        name="combine",
    )(slot_ids, route_weight, returned, shared)


def body(
    mixer_input,
    mixer_gain,
    query_one,
    query_two,
    key_one,
    key_two,
    value_weight,
    lambdas,
    head_gain,
    output_weight,
    expert_input,
    expert_gain,
    routes,
    route_weight,
    expert_gate,
    expert_up,
    expert_down,
    shared_gate,
    shared_up,
    shared_down,
):
    ep_size = lax.axis_size("ep")
    tp_size = lax.axis_size("tp")
    ep_rank = lax.axis_index("ep")
    query_cols = query_one.shape[1]
    key_cols = key_one.shape[1]
    local_kv = key_cols // HEAD
    group = query_cols // key_cols
    experts_local = expert_gate.shape[0]

    gates = tp_blocks(expert_gate, tp_size)
    ups = tp_blocks(expert_up, tp_size)
    downs = tp_blocks(expert_down, tp_size)

    token_rows, model_width = expert_input.shape
    normed_experts = normalize(expert_input, expert_gain)
    expert_count = experts_local * ep_size
    top_count = routes.shape[1]
    capacity = max(2, 5 * token_rows * top_count // (4 * expert_count))
    slot_count = expert_count * capacity
    relative = (routes - ep_rank * experts_local) % expert_count
    flat_routes = relative.reshape(-1)
    onehot = (flat_routes[:, None] == jnp.arange(expert_count, dtype=jnp.int32)[None, :]).astype(
        jnp.int32
    )
    slot_place = jnp.sum((jnp.cumsum(onehot, axis=0) - onehot) * onehot, axis=1)
    slot_ids = (flat_routes * capacity + slot_place).reshape(token_rows, top_count)
    slot_match = jnp.arange(slot_count, dtype=jnp.int32)[:, None, None] == slot_ids[None, :, :]
    select = jnp.any(slot_match, axis=2).astype(jnp.bfloat16)
    outgoing = jnp.dot(select, normed_experts, preferred_element_type=jnp.float32).astype(
        jnp.bfloat16
    )
    outgoing, normed_experts = lax.optimization_barrier((outgoing, normed_experts))
    expert_rows = lax.all_gather(normed_experts, "tp", axis=0, tiled=True)
    span = experts_local * capacity
    received = exchange(
        [outgoing[k * span : (k + 1) * span] for k in range(ep_size)], ep_rank, ep_size, 1
    )

    normed = normalize(mixer_input, mixer_gain)
    joined_weight = jnp.concatenate([query_one, query_two, key_one, key_two, value_weight], axis=1)
    projected = jnp.dot(normed, joined_weight, preferred_element_type=jnp.float32).astype(
        jnp.bfloat16
    )
    queries = projected[:, : 2 * query_cols]
    key_values = projected[:, 2 * query_cols :]
    if ep_size <= MOST_PERMUTES:
        others = jnp.stack(
            [
                lax.ppermute(key_values, "ep", [(i, i + k) for i in range(ep_size - k)])
                for k in range(1, ep_size)
            ]
        )
    else:
        others = lax.all_gather(key_values, "ep", axis=0)
    mixer_part = attention(
        ep_rank, lambdas, queries, key_values, others, head_gain, output_weight, local_kv, group
    )
    mixer_sum = lax.psum_scatter(mixer_part, "tp", scatter_dimension=0, tiled=True)

    shared_gated = jnp.dot(expert_rows, shared_gate, preferred_element_type=jnp.float32)
    shared_lifted = jnp.dot(expert_rows, shared_up, preferred_element_type=jnp.float32)
    shared_hidden = (jax.nn.silu(shared_gated) * shared_lifted).astype(jnp.bfloat16)
    shared_part = jnp.dot(shared_hidden, shared_down, preferred_element_type=jnp.float32)
    shared_sum = lax.psum_scatter(
        shared_part.astype(jnp.bfloat16), "tp", scatter_dimension=0, tiled=True
    )

    slot_rows = jnp.concatenate(received, axis=0).reshape(
        ep_size, experts_local, capacity, model_width
    )
    results = []
    for e in range(experts_local):
        rows = slot_rows[:, e].reshape(ep_size * capacity, model_width)
        total = jnp.zeros((ep_size * capacity, model_width), jnp.float32)
        for gate, up, down in zip(gates, ups, downs):
            gated = jnp.dot(rows, gate[e], preferred_element_type=jnp.float32)
            lifted = jnp.dot(rows, up[e], preferred_element_type=jnp.float32)
            hidden = (jax.nn.silu(gated) * lifted).astype(jnp.bfloat16)
            partial = jnp.dot(hidden, down[e], preferred_element_type=jnp.float32)
            total = total + partial.astype(jnp.bfloat16).astype(jnp.float32)
        results.append(total.astype(jnp.bfloat16).reshape(ep_size, 1, capacity, model_width))
    routed = jnp.concatenate(results, axis=1).reshape(ep_size, span, model_width)
    returned = exchange([routed[k] for k in range(ep_size)], ep_rank, ep_size, -1)
    expert_output = combine(
        slot_ids, route_weight, jnp.concatenate(returned, axis=0), shared_sum
    )
    return (mixer_sum, expert_output)


def solution(mesh):
    in_specs = (
        P("ep", None),
        P(),
        P(None, "tp"),
        P(None, "tp"),
        P(None, "tp"),
        P(None, "tp"),
        P(None, "tp"),
        P("tp"),
        P(),
        P("tp", None),
        P(("ep", "tp"), None),
        P(),
        P(("ep", "tp"), None),
        P(("ep", "tp"), None),
        P("ep", None, "tp"),
        P("ep", None, "tp"),
        P("ep", "tp", None),
        P(None, "tp"),
        P(None, "tp"),
        P("tp", None),
    )
    out_specs = (P(("ep", "tp"), None), P(("ep", "tp"), None))
    return jax.shard_map(body, mesh=mesh, in_specs=in_specs, out_specs=out_specs, check_vma=False)
```

```python
import jax
import jax.numpy as jnp
from jax import lax
from jax.experimental import pallas as pl
from jax.experimental.pallas import tpu as pltpu
from jax.sharding import PartitionSpec as P


HEAD = 64
EPS = 1e-06
NEG = -1e30
MOST_PERMUTES = 8


def normalize(activations, scaling):
    values = activations.astype(jnp.float32)
    factor = lax.rsqrt(jnp.mean(values * values, axis=-1, keepdims=True) + EPS)
    return (values * factor * scaling).astype(jnp.bfloat16)


def rotate(chunk, axis, size, shift):
    return lax.ppermute(chunk, axis, [(i, (i + shift) % size) for i in range(size)])


def exchange(chunks, rank, size, sign):
    if size <= MOST_PERMUTES:
        return [chunks[0]] + [
            rotate(chunk, "ep", size, sign * k) for k, chunk in enumerate(chunks) if k
        ]
    order = (sign * (jnp.arange(size, dtype=jnp.int32) - rank)) % size
    arrived = lax.all_to_all(
        jnp.stack(chunks)[order], "ep", split_axis=0, concat_axis=0, tiled=True
    )
    back = (rank - sign * jnp.arange(size, dtype=jnp.int32)) % size
    arrived = arrived[back]
    return [arrived.reshape(-1, arrived.shape[-1])]


VMEM = pl.BlockSpec(memory_space=pltpu.VMEM)
SMEM = pl.BlockSpec(memory_space=pltpu.SMEM)


def project_kernel(rows_ref, gain_ref, one, two, key_one, key_two, value, query_ref, kv_ref):
    values = rows_ref[...].astype(jnp.float32)
    factor = lax.rsqrt(jnp.mean(values * values, axis=-1, keepdims=True) + EPS)
    normed = (values * factor * gain_ref[...]).astype(jnp.bfloat16)

    def plain(weight):
        return jnp.dot(normed, weight[...], preferred_element_type=jnp.float32).astype(jnp.bfloat16)

    def turned(weight):
        return lax.dot_general(
            normed, weight[...], (((1,), (1,)), ((), ())), preferred_element_type=jnp.float32
        ).astype(jnp.bfloat16)

    query_ref[...] = jnp.concatenate([plain(one), plain(two)], axis=1)
    kv_ref[...] = jnp.concatenate([turned(key_one), turned(key_two), plain(value)], axis=1)


def project(rows, gain, one, two, key_one, key_two, value):
    count = rows.shape[0]
    kv_cols = 2 * key_one.shape[1] + value.shape[1]
    return pl.pallas_call(
        project_kernel,
        out_shape=(
            jax.ShapeDtypeStruct((count, 2 * one.shape[1]), jnp.bfloat16),
            jax.ShapeDtypeStruct((count, kv_cols), jnp.bfloat16),
        ),
        in_specs=[VMEM] * 7,
        out_specs=(VMEM, VMEM),
        cost_estimate=pl.CostEstimate(
            flops=2_000_000_000, transcendentals=1000, bytes_accessed=4_000_000
        ),
        name="project",
    )(rows, gain.reshape(1, -1), one, two, key_one.T, key_two.T, value)


def stack(chunks):
    if len(chunks) == 1:
        return chunks[0]
    rows, width = chunks[0].shape

    def kernel(*refs):
        for k, ref in enumerate(refs[:-1]):
            refs[-1][k] = ref[...]

    return pl.pallas_call(
        kernel,
        out_shape=jax.ShapeDtypeStruct((len(chunks), rows, width), chunks[0].dtype),
        in_specs=[VMEM] * len(chunks),
        out_specs=VMEM,
        name="stack",
    )(*chunks).reshape(-1, width)


def routed_part(rows, gates, ups, downs, earlier, last):
    count = len(gates)

    def kernel(*refs):
        rows_ref, out_ref = refs[0], refs[-1]
        gate_refs = refs[1 : 1 + count]
        up_refs = refs[1 + count : 1 + 2 * count]
        down_refs = refs[1 + 2 * count : 1 + 3 * count]
        inputs = rows_ref[...]
        hidden = []
        for gate, up in zip(gate_refs, up_refs):
            gated = jnp.dot(inputs, gate[...], preferred_element_type=jnp.float32)
            lifted = jnp.dot(inputs, up[...], preferred_element_type=jnp.float32)
            hidden.append((jax.nn.silu(gated) * lifted).astype(jnp.bfloat16))
        total = None if earlier is None else refs[1 + 3 * count][...]
        for units, down in zip(hidden, down_refs):
            part = jnp.dot(units, down[...], preferred_element_type=jnp.float32)
            part = part.astype(jnp.bfloat16).astype(jnp.float32)
            total = part if total is None else total + part
        out_ref[...] = total.astype(out_ref.dtype)

    operands = [rows, *gates, *ups, *downs] + ([] if earlier is None else [earlier])
    return pl.pallas_call(
        kernel,
        out_shape=jax.ShapeDtypeStruct(rows.shape, jnp.bfloat16 if last else jnp.float32),
        in_specs=[VMEM] * len(operands),
        out_specs=VMEM,
        cost_estimate=pl.CostEstimate(
            flops=count * 2_000_000_000, transcendentals=1000, bytes_accessed=8_000_000
        ),
        compiler_params=pltpu.CompilerParams(vmem_limit_bytes=48 * 1024 * 1024),
        name="routed",
    )(*operands)


def tp_blocks(shard, size):
    blocks = [shard]
    bit = size // 2
    while bit:
        pairs = [(i, i ^ bit) for i in range(size)]
        blocks = blocks + [lax.ppermute(block, "tp", pairs) for block in blocks]
        bit //= 2
    return blocks


def attention_kernel(
    rank_ref,
    lambda_ref,
    query_ref,
    own_ref,
    gain_ref,
    weight_ref,
    *rest,
    local_kv,
    group,
    value_dim,
):
    out_ref, maxima, totals, weighted = rest[-4:]
    others = rest[:-4]
    rows = query_ref.shape[0]
    key_cols = local_kv * HEAD
    query_cols = key_cols * group

    def stacked(head, which):
        first = which * query_cols + head * group * HEAD
        return jnp.concatenate(
            [query_ref[:, first + g * HEAD : first + (g + 1) * HEAD] for g in range(group)], axis=0
        ) * jnp.bfloat16(HEAD ** (-0.5))

    queries = [[stacked(head, which) for which in range(2)] for head in range(local_kv)]

    def block(keys, head, which):
        key_part = keys[:, which * key_cols + head * HEAD : which * key_cols + (head + 1) * HEAD]
        value_part = keys[
            :, 2 * key_cols + head * value_dim : 2 * key_cols + (head + 1) * value_dim
        ]
        scores = lax.dot_general(
            queries[head][which],
            key_part,
            (((1,), (1,)), ((), ())),
            preferred_element_type=jnp.float32,
        )
        return scores, value_part

    own = own_ref[...]
    position = lax.broadcasted_iota(jnp.int32, (group * rows, rows), 0) % rows
    visible = lax.broadcasted_iota(jnp.int32, (group * rows, rows), 1) <= position
    for head in range(local_kv):
        for which in range(2):
            slot = head * 2 + which
            scores, value_part = block(own, head, which)
            scores = jnp.where(visible, scores, NEG)
            highest = jnp.max(scores, axis=-1, keepdims=True)
            weights = jnp.exp(scores - highest)
            maxima[slot] = highest
            totals[slot] = jnp.sum(weights, axis=-1, keepdims=True)
            weighted[slot] = jnp.dot(
                weights.astype(jnp.bfloat16), value_part, preferred_element_type=jnp.float32
            )

    def earlier_block(keys):
        for head in range(local_kv):
            for which in range(2):
                slot = head * 2 + which
                scores, value_part = block(keys, head, which)
                before = maxima[slot]
                highest = jnp.maximum(before, jnp.max(scores, axis=-1, keepdims=True))
                shrink = jnp.exp(before - highest)
                weights = jnp.exp(scores - highest)
                maxima[slot] = highest
                totals[slot] = totals[slot] * shrink + jnp.sum(weights, axis=-1, keepdims=True)
                weighted[slot] = weighted[slot] * shrink + jnp.dot(
                    weights.astype(jnp.bfloat16), value_part, preferred_element_type=jnp.float32
                )

    if len(others) > 1:
        for step, other in enumerate(others):
            pl.when(step < rank_ref[0])(lambda other=other: earlier_block(other[...]))
    else:

        def one_step(step, carry):
            earlier_block(others[0][step])
            return carry

        lax.fori_loop(0, rank_ref[0], one_step, 0)
    parts = []
    for head in range(local_kv):
        first = weighted[head * 2] / totals[head * 2]
        second = weighted[head * 2 + 1] / totals[head * 2 + 1]
        for g in range(group):
            span = slice(g * rows, (g + 1) * rows)
            combined = first[span] - lambda_ref[head * group + g] * second[span]
            factor = lax.rsqrt(jnp.mean(combined * combined, axis=-1, keepdims=True) + EPS)
            parts.append((combined * factor * gain_ref[...]).astype(jnp.bfloat16))
    head_rows = jnp.concatenate(parts, axis=1)
    out_ref[...] = jnp.dot(
        head_rows, weight_ref[...], preferred_element_type=jnp.float32
    ).astype(jnp.bfloat16)


def attention(rank, lambdas, queries, own, others, head_gain, output_weight, local_kv, group):
    rows = queries.shape[0]
    value_dim = head_gain.shape[0]
    kernel = lambda *refs: attention_kernel(
        *refs, local_kv=local_kv, group=group, value_dim=value_dim
    )
    stats = (2 * local_kv, group * rows, 1)
    return pl.pallas_call(
        kernel,
        out_shape=jax.ShapeDtypeStruct((rows, output_weight.shape[1]), jnp.bfloat16),
        in_specs=[SMEM, SMEM] + [VMEM] * (4 + len(others)),
        out_specs=VMEM,
        scratch_shapes=[
            pltpu.VMEM(stats, jnp.float32),
            pltpu.VMEM(stats, jnp.float32),
            pltpu.VMEM((2 * local_kv, group * rows, value_dim), jnp.float32),
        ],
        cost_estimate=pl.CostEstimate(
            flops=6_000_000_000, transcendentals=4_000_000, bytes_accessed=4_000_000
        ),
        name="attention",
    )(rank.reshape(1), lambdas, queries, own, head_gain.reshape(1, -1), output_weight, *others)


def combine_kernel(slot_ref, weight_ref, shared_ref, *rest):
    out_ref = rest[-1]
    returned = rest[0][...] if len(rest) == 2 else jnp.concatenate([r[...] for r in rest[:-1]], 0)
    tokens, top = slot_ref.shape
    places = lax.broadcasted_iota(jnp.int32, (tokens, returned.shape[0]), 1)
    total = shared_ref[...].astype(jnp.float32)
    for k in range(top):
        chosen = (places == slot_ref[:, k : k + 1]).astype(jnp.float32).astype(jnp.bfloat16)
        picked = jnp.dot(chosen, returned, preferred_element_type=jnp.float32)
        total = total + picked * weight_ref[:, k : k + 1]
    out_ref[...] = total.astype(jnp.bfloat16)


def combine(slot_ids, route_weight, returned, shared):
    tokens, width = shared.shape
    top = slot_ids.shape[1]
    cols = width // 2
    return pl.pallas_call(
        combine_kernel,
        grid=(width // cols,),
        out_shape=jax.ShapeDtypeStruct((tokens, width), jnp.bfloat16),
        in_specs=[
            pl.BlockSpec((tokens, top), lambda i: (0, 0)),
            pl.BlockSpec((tokens, top), lambda i: (0, 0)),
            pl.BlockSpec((tokens, cols), lambda i: (0, i)),
        ]
        + [pl.BlockSpec((chunk.shape[0], cols), lambda i: (0, i)) for chunk in returned],
        out_specs=pl.BlockSpec((tokens, cols), lambda i: (0, i)),
        name="combine",
    )(slot_ids, route_weight, shared, *returned)


def body(
    mixer_input,
    mixer_gain,
    query_one,
    query_two,
    key_one,
    key_two,
    value_weight,
    lambdas,
    head_gain,
    output_weight,
    expert_input,
    expert_gain,
    routes,
    route_weight,
    expert_gate,
    expert_up,
    expert_down,
    shared_gate,
    shared_up,
    shared_down,
):
    ep_size = lax.axis_size("ep")
    tp_size = lax.axis_size("tp")
    ep_rank = lax.axis_index("ep")
    query_cols = query_one.shape[1]
    key_cols = key_one.shape[1]
    local_kv = key_cols // HEAD
    group = query_cols // key_cols
    experts_local = expert_gate.shape[0]

    gates = tp_blocks(expert_gate, tp_size)
    ups = tp_blocks(expert_up, tp_size)
    downs = tp_blocks(expert_down, tp_size)

    token_rows, model_width = expert_input.shape
    normed_experts = normalize(expert_input, expert_gain)
    expert_count = experts_local * ep_size
    top_count = routes.shape[1]
    capacity = max(2, 5 * token_rows * top_count // (4 * expert_count))
    slot_count = expert_count * capacity
    relative = (routes - ep_rank * experts_local) % expert_count
    flat_routes = relative.reshape(-1)
    onehot = (flat_routes[:, None] == jnp.arange(expert_count, dtype=jnp.int32)[None, :]).astype(
        jnp.int32
    )
    slot_place = jnp.sum((jnp.cumsum(onehot, axis=0) - onehot) * onehot, axis=1)
    slot_ids = (flat_routes * capacity + slot_place).reshape(token_rows, top_count)
    slot_match = jnp.arange(slot_count, dtype=jnp.int32)[:, None, None] == slot_ids[None, :, :]
    select = jnp.any(slot_match, axis=2).astype(jnp.bfloat16)
    outgoing = jnp.dot(select, normed_experts, preferred_element_type=jnp.float32).astype(
        jnp.bfloat16
    )
    outgoing, normed_experts = lax.optimization_barrier((outgoing, normed_experts))
    expert_rows = lax.all_gather(normed_experts, "tp", axis=0, tiled=True)
    span = experts_local * capacity
    received = exchange(
        [outgoing[k * span : (k + 1) * span] for k in range(ep_size)], ep_rank, ep_size, 1
    )

    queries, key_values = project(
        mixer_input, mixer_gain, query_one, query_two, key_one, key_two, value_weight
    )
    if ep_size <= MOST_PERMUTES:
        others = [
            lax.ppermute(key_values, "ep", [(i, i + k) for i in range(ep_size - k)])
            for k in range(1, ep_size)
        ]
    else:
        others = [lax.all_gather(key_values, "ep", axis=0)]
    mixer_part = attention(
        ep_rank, lambdas, queries, key_values, others, head_gain, output_weight, local_kv, group
    )
    mixer_sum = lax.psum_scatter(mixer_part, "tp", scatter_dimension=0, tiled=True)

    shared_gated = jnp.dot(expert_rows, shared_gate, preferred_element_type=jnp.float32)
    shared_lifted = jnp.dot(expert_rows, shared_up, preferred_element_type=jnp.float32)
    shared_hidden = (jax.nn.silu(shared_gated) * shared_lifted).astype(jnp.bfloat16)
    shared_part = jnp.dot(shared_hidden, shared_down, preferred_element_type=jnp.float32)
    shared_sum = lax.psum_scatter(
        shared_part.astype(jnp.bfloat16), "tp", scatter_dimension=0, tiled=True
    )

    slot_rows = stack(received).reshape(ep_size, experts_local, capacity, model_width)
    half = max(1, tp_size // 2)
    order = [0, half] + [k for k in range(1, tp_size) if k != half] if tp_size > 1 else [0]
    results = []
    for e in range(experts_local):
        rows = slot_rows[:, e].reshape(ep_size * capacity, model_width)
        total = None
        for first in range(0, len(order), 2):
            part = order[first : first + 2]
            total = routed_part(
                rows,
                [gates[k][e] for k in part],
                [ups[k][e] for k in part],
                [downs[k][e] for k in part],
                total,
                first + 2 >= len(order),
            )
        results.append(total.reshape(ep_size, 1, capacity, model_width))
    routed = jnp.concatenate(results, axis=1).reshape(ep_size, span, model_width)
    returned = exchange([routed[k] for k in range(ep_size)], ep_rank, ep_size, -1)
    expert_output = combine(slot_ids, route_weight, returned, shared_sum)
    return (mixer_sum, expert_output)


def solution(mesh):
    in_specs = (
        P("ep", None),
        P(),
        P(None, "tp"),
        P(None, "tp"),
        P(None, "tp"),
        P(None, "tp"),
        P(None, "tp"),
        P("tp"),
        P(),
        P("tp", None),
        P(("ep", "tp"), None),
        P(),
        P(("ep", "tp"), None),
        P(("ep", "tp"), None),
        P("ep", None, "tp"),
        P("ep", None, "tp"),
        P("ep", "tp", None),
        P(None, "tp"),
        P(None, "tp"),
        P("tp", None),
    )
    out_specs = (P(("ep", "tp"), None), P(("ep", "tp"), None))

    return jax.shard_map(body, mesh=mesh, in_specs=in_specs, out_specs=out_specs, check_vma=False)
```

```python
import jax
import jax.numpy as jnp
from jax import lax
from jax.experimental import pallas as pl
from jax.experimental.pallas import tpu as pltpu
from jax.sharding import PartitionSpec as P


HEAD = 64
EPS = 1e-06
NEG = -1e30
MOST_PERMUTES = 8


def normalize(activations, scaling):
    values = activations.astype(jnp.float32)
    factor = lax.rsqrt(jnp.mean(values * values, axis=-1, keepdims=True) + EPS)
    return (values * factor * scaling).astype(jnp.bfloat16)


def rotate(chunk, axis, size, shift):
    return lax.ppermute(chunk, axis, [(i, (i + shift) % size) for i in range(size)])


def exchange(chunks, rank, size, sign):
    if size <= MOST_PERMUTES:
        return [chunks[0]] + [
            rotate(chunk, "ep", size, sign * k) for k, chunk in enumerate(chunks) if k
        ]
    order = (sign * (jnp.arange(size, dtype=jnp.int32) - rank)) % size
    arrived = lax.all_to_all(
        jnp.stack(chunks)[order], "ep", split_axis=0, concat_axis=0, tiled=True
    )
    back = (rank - sign * jnp.arange(size, dtype=jnp.int32)) % size
    arrived = arrived[back]
    return [arrived.reshape(-1, arrived.shape[-1])]


VMEM = pl.BlockSpec(memory_space=pltpu.VMEM)
SMEM = pl.BlockSpec(memory_space=pltpu.SMEM)


def project_kernel(rows_ref, gain_ref, one, two, key_one, key_two, value, query_ref, kv_ref):
    values = rows_ref[...].astype(jnp.float32)
    factor = lax.rsqrt(jnp.mean(values * values, axis=-1, keepdims=True) + EPS)
    normed = (values * factor * gain_ref[...]).astype(jnp.bfloat16)

    def plain(weight):
        return jnp.dot(normed, weight[...], preferred_element_type=jnp.float32).astype(jnp.bfloat16)

    def turned(weight):
        return lax.dot_general(
            normed, weight[...], (((1,), (1,)), ((), ())), preferred_element_type=jnp.float32
        ).astype(jnp.bfloat16)

    query_ref[...] = jnp.concatenate([plain(one), plain(two)], axis=1)
    kv_ref[...] = jnp.concatenate([turned(key_one), turned(key_two), plain(value)], axis=1)


def project(rows, gain, one, two, key_one, key_two, value):
    count = rows.shape[0]
    kv_cols = 2 * key_one.shape[1] + value.shape[1]
    return pl.pallas_call(
        project_kernel,
        out_shape=(
            jax.ShapeDtypeStruct((count, 2 * one.shape[1]), jnp.bfloat16),
            jax.ShapeDtypeStruct((count, kv_cols), jnp.bfloat16),
        ),
        in_specs=[VMEM] * 7,
        out_specs=(VMEM, VMEM),
        cost_estimate=pl.CostEstimate(
            flops=2_000_000_000, transcendentals=1000, bytes_accessed=4_000_000
        ),
        name="project",
    )(rows, gain.reshape(1, -1), one, two, key_one.T, key_two.T, value)


def stack(chunks):
    if len(chunks) == 1:
        return chunks[0]
    rows, width = chunks[0].shape

    def kernel(*refs):
        for k, ref in enumerate(refs[:-1]):
            refs[-1][k] = ref[...]

    return pl.pallas_call(
        kernel,
        out_shape=jax.ShapeDtypeStruct((len(chunks), rows, width), chunks[0].dtype),
        in_specs=[VMEM] * len(chunks),
        out_specs=VMEM,
        name="stack",
    )(*chunks).reshape(-1, width)


def routed_part(rows, gates, ups, downs, earlier, last):
    count = len(gates)

    def kernel(*refs):
        rows_ref, out_ref = refs[0], refs[-1]
        gate_refs = refs[1 : 1 + count]
        up_refs = refs[1 + count : 1 + 2 * count]
        down_refs = refs[1 + 2 * count : 1 + 3 * count]
        inputs = rows_ref[...]
        hidden = []
        for gate, up in zip(gate_refs, up_refs):
            gated = jnp.dot(inputs, gate[...], preferred_element_type=jnp.float32)
            lifted = jnp.dot(inputs, up[...], preferred_element_type=jnp.float32)
            hidden.append((jax.nn.silu(gated) * lifted).astype(jnp.bfloat16))
        total = None if earlier is None else refs[1 + 3 * count][...]
        for units, down in zip(hidden, down_refs):
            part = jnp.dot(units, down[...], preferred_element_type=jnp.float32)
            part = part.astype(jnp.bfloat16).astype(jnp.float32)
            total = part if total is None else total + part
        out_ref[...] = total.astype(out_ref.dtype)

    operands = [rows, *gates, *ups, *downs] + ([] if earlier is None else [earlier])
    return pl.pallas_call(
        kernel,
        out_shape=jax.ShapeDtypeStruct(rows.shape, jnp.bfloat16 if last else jnp.float32),
        in_specs=[VMEM] * len(operands),
        out_specs=VMEM,
        cost_estimate=pl.CostEstimate(
            flops=count * 2_000_000_000, transcendentals=1000, bytes_accessed=8_000_000
        ),
        compiler_params=pltpu.CompilerParams(vmem_limit_bytes=48 * 1024 * 1024),
        name="routed",
    )(*operands)


def tp_blocks(shard, size):
    blocks = [shard]
    bit = size // 2
    while bit:
        pairs = [(i, i ^ bit) for i in range(size)]
        blocks = blocks + [lax.ppermute(block, "tp", pairs) for block in blocks]
        bit //= 2
    return blocks


def attention_kernel(
    rank_ref,
    lambda_ref,
    query_ref,
    own_ref,
    gain_ref,
    weight_ref,
    *rest,
    local_kv,
    group,
    value_dim,
):
    out_ref, maxima, totals, weighted = rest[-4:]
    others = rest[:-4]
    rows = query_ref.shape[0]
    key_cols = local_kv * HEAD
    query_cols = key_cols * group

    def stacked(head, which):
        first = which * query_cols + head * group * HEAD
        return jnp.concatenate(
            [query_ref[:, first + g * HEAD : first + (g + 1) * HEAD] for g in range(group)], axis=0
        ) * jnp.bfloat16(HEAD ** (-0.5))

    queries = [[stacked(head, which) for which in range(2)] for head in range(local_kv)]

    def block(keys, head, which):
        key_part = keys[:, which * key_cols + head * HEAD : which * key_cols + (head + 1) * HEAD]
        value_part = keys[
            :, 2 * key_cols + head * value_dim : 2 * key_cols + (head + 1) * value_dim
        ]
        scores = lax.dot_general(
            queries[head][which],
            key_part,
            (((1,), (1,)), ((), ())),
            preferred_element_type=jnp.float32,
        )
        return scores, value_part

    own = own_ref[...]
    position = lax.broadcasted_iota(jnp.int32, (group * rows, rows), 0) % rows
    visible = lax.broadcasted_iota(jnp.int32, (group * rows, rows), 1) <= position
    for head in range(local_kv):
        for which in range(2):
            slot = head * 2 + which
            scores, value_part = block(own, head, which)
            scores = jnp.where(visible, scores, NEG)
            highest = jnp.max(scores, axis=-1, keepdims=True)
            weights = jnp.exp(scores - highest)
            maxima[slot] = highest
            totals[slot] = jnp.sum(weights, axis=-1, keepdims=True)
            weighted[slot] = jnp.dot(
                weights.astype(jnp.bfloat16), value_part, preferred_element_type=jnp.float32
            )

    def earlier_block(keys):
        for head in range(local_kv):
            for which in range(2):
                slot = head * 2 + which
                scores, value_part = block(keys, head, which)
                before = maxima[slot]
                highest = jnp.maximum(before, jnp.max(scores, axis=-1, keepdims=True))
                shrink = jnp.exp(before - highest)
                weights = jnp.exp(scores - highest)
                maxima[slot] = highest
                totals[slot] = totals[slot] * shrink + jnp.sum(weights, axis=-1, keepdims=True)
                weighted[slot] = weighted[slot] * shrink + jnp.dot(
                    weights.astype(jnp.bfloat16), value_part, preferred_element_type=jnp.float32
                )

    if len(others) > 1:
        for step, other in enumerate(others):
            pl.when(step < rank_ref[0])(lambda other=other: earlier_block(other[...]))
    else:

        def one_step(step, carry):
            earlier_block(others[0][step])
            return carry

        lax.fori_loop(0, rank_ref[0], one_step, 0)
    parts = []
    for head in range(local_kv):
        first = weighted[head * 2] / totals[head * 2]
        second = weighted[head * 2 + 1] / totals[head * 2 + 1]
        for g in range(group):
            span = slice(g * rows, (g + 1) * rows)
            combined = first[span] - lambda_ref[head * group + g] * second[span]
            factor = lax.rsqrt(jnp.mean(combined * combined, axis=-1, keepdims=True) + EPS)
            parts.append((combined * factor * gain_ref[...]).astype(jnp.bfloat16))
    head_rows = jnp.concatenate(parts, axis=1)
    out_ref[...] = jnp.dot(
        head_rows, weight_ref[...], preferred_element_type=jnp.float32
    ).astype(jnp.bfloat16)


def attention(rank, lambdas, queries, own, others, head_gain, output_weight, local_kv, group):
    rows = queries.shape[0]
    value_dim = head_gain.shape[0]
    kernel = lambda *refs: attention_kernel(
        *refs, local_kv=local_kv, group=group, value_dim=value_dim
    )
    stats = (2 * local_kv, group * rows, 1)
    return pl.pallas_call(
        kernel,
        out_shape=jax.ShapeDtypeStruct((rows, output_weight.shape[1]), jnp.bfloat16),
        in_specs=[SMEM, SMEM] + [VMEM] * (4 + len(others)),
        out_specs=VMEM,
        scratch_shapes=[
            pltpu.VMEM(stats, jnp.float32),
            pltpu.VMEM(stats, jnp.float32),
            pltpu.VMEM((2 * local_kv, group * rows, value_dim), jnp.float32),
        ],
        cost_estimate=pl.CostEstimate(
            flops=6_000_000_000, transcendentals=4_000_000, bytes_accessed=4_000_000
        ),
        name="attention",
    )(rank.reshape(1), lambdas, queries, own, head_gain.reshape(1, -1), output_weight, *others)


def combine_kernel(slot_ref, weight_ref, shared_ref, *rest):
    out_ref = rest[-1]
    returned = rest[0][...] if len(rest) == 2 else jnp.concatenate([r[...] for r in rest[:-1]], 0)
    tokens, top = slot_ref.shape
    places = lax.broadcasted_iota(jnp.int32, (tokens, returned.shape[0]), 1)
    total = shared_ref[...].astype(jnp.float32)
    for k in range(top):
        chosen = (places == slot_ref[:, k : k + 1]).astype(jnp.float32).astype(jnp.bfloat16)
        picked = jnp.dot(chosen, returned, preferred_element_type=jnp.float32)
        total = total + picked * weight_ref[:, k : k + 1]
    out_ref[...] = total.astype(jnp.bfloat16)


def combine(slot_ids, route_weight, returned, shared):
    tokens, width = shared.shape
    top = slot_ids.shape[1]
    cols = width // 2
    return pl.pallas_call(
        combine_kernel,
        grid=(width // cols,),
        out_shape=jax.ShapeDtypeStruct((tokens, width), jnp.bfloat16),
        in_specs=[
            pl.BlockSpec((tokens, top), lambda i: (0, 0)),
            pl.BlockSpec((tokens, top), lambda i: (0, 0)),
            pl.BlockSpec((tokens, cols), lambda i: (0, i)),
        ]
        + [pl.BlockSpec((chunk.shape[0], cols), lambda i: (0, i)) for chunk in returned],
        out_specs=pl.BlockSpec((tokens, cols), lambda i: (0, i)),
        name="combine",
    )(slot_ids, route_weight, shared, *returned)


def body(
    mixer_input,
    mixer_gain,
    query_one,
    query_two,
    key_one,
    key_two,
    value_weight,
    lambdas,
    head_gain,
    output_weight,
    expert_input,
    expert_gain,
    routes,
    route_weight,
    expert_gate,
    expert_up,
    expert_down,
    shared_gate,
    shared_up,
    shared_down,
):
    ep_size = lax.axis_size("ep")
    tp_size = lax.axis_size("tp")
    ep_rank = lax.axis_index("ep")
    query_cols = query_one.shape[1]
    key_cols = key_one.shape[1]
    local_kv = key_cols // HEAD
    group = query_cols // key_cols
    experts_local = expert_gate.shape[0]

    gates = tp_blocks(expert_gate, tp_size)
    ups = tp_blocks(expert_up, tp_size)
    downs = tp_blocks(expert_down, tp_size)
    shared_weights = [
        tp_blocks(weight, tp_size) for weight in (shared_gate, shared_up, shared_down)
    ]

    token_rows, model_width = expert_input.shape
    normed_experts = normalize(expert_input, expert_gain)
    expert_count = experts_local * ep_size
    top_count = routes.shape[1]
    capacity = max(2, 5 * token_rows * top_count // (4 * expert_count))
    slot_count = expert_count * capacity
    relative = (routes - ep_rank * experts_local) % expert_count
    flat_routes = relative.reshape(-1)
    onehot = (flat_routes[:, None] == jnp.arange(expert_count, dtype=jnp.int32)[None, :]).astype(
        jnp.int32
    )
    slot_place = jnp.sum((jnp.cumsum(onehot, axis=0) - onehot) * onehot, axis=1)
    slot_ids = (flat_routes * capacity + slot_place).reshape(token_rows, top_count)
    slot_match = jnp.arange(slot_count, dtype=jnp.int32)[:, None, None] == slot_ids[None, :, :]
    select = jnp.any(slot_match, axis=2).astype(jnp.bfloat16)
    outgoing = jnp.dot(select, normed_experts, preferred_element_type=jnp.float32).astype(
        jnp.bfloat16
    )
    span = experts_local * capacity
    received = exchange(
        [outgoing[k * span : (k + 1) * span] for k in range(ep_size)], ep_rank, ep_size, 1
    )

    queries, key_values = project(
        mixer_input, mixer_gain, query_one, query_two, key_one, key_two, value_weight
    )
    if ep_size <= MOST_PERMUTES:
        others = [
            lax.ppermute(key_values, "ep", [(i, i + k) for i in range(ep_size - k)])
            for k in range(1, ep_size)
        ]
    else:
        others = [lax.all_gather(key_values, "ep", axis=0)]
    mixer_part = attention(
        ep_rank, lambdas, queries, key_values, others, head_gain, output_weight, local_kv, group
    )
    mixer_sum = lax.psum_scatter(mixer_part, "tp", scatter_dimension=0, tiled=True)

    shared_sum = routed_part(normed_experts, *shared_weights, None, False)

    slot_rows = stack(received).reshape(ep_size, experts_local, capacity, model_width)
    half = max(1, tp_size // 2)
    order = [0, half] + [k for k in range(1, tp_size) if k != half] if tp_size > 1 else [0]
    results = []
    for e in range(experts_local):
        rows = slot_rows[:, e].reshape(ep_size * capacity, model_width)
        total = None
        for first in range(0, len(order), 2):
            part = order[first : first + 2]
            total = routed_part(
                rows,
                [gates[k][e] for k in part],
                [ups[k][e] for k in part],
                [downs[k][e] for k in part],
                total,
                first + 2 >= len(order),
            )
        results.append(total.reshape(ep_size, 1, capacity, model_width))
    routed = jnp.concatenate(results, axis=1).reshape(ep_size, span, model_width)
    returned = exchange([routed[k] for k in range(ep_size)], ep_rank, ep_size, -1)
    expert_output = combine(slot_ids, route_weight, returned, shared_sum)
    return (mixer_sum, expert_output)


def solution(mesh):
    in_specs = (
        P("ep", None),
        P(),
        P(None, "tp"),
        P(None, "tp"),
        P(None, "tp"),
        P(None, "tp"),
        P(None, "tp"),
        P("tp"),
        P(),
        P("tp", None),
        P(("ep", "tp"), None),
        P(),
        P(("ep", "tp"), None),
        P(("ep", "tp"), None),
        P("ep", None, "tp"),
        P("ep", None, "tp"),
        P("ep", "tp", None),
        P(None, "tp"),
        P(None, "tp"),
        P("tp", None),
    )
    out_specs = (P(("ep", "tp"), None), P(("ep", "tp"), None))

    return jax.shard_map(body, mesh=mesh, in_specs=in_specs, out_specs=out_specs, check_vma=False)
```
